256 devices in a mesh: grp: 2 (over y), sp: 32 (over z, core), tp: 4 (over x).
Axes of the slice: x: 4, y: 2, z: 16, core: 2. Of those that a mesh axis runs over, the one named last changes fastest.
The devices are a block of a 4x16x16 slice.
Arguments:
- queries: bfloat16 [16384, 2048], P(('grp', 'sp'), 'tp'), parts along dimension 0, may hold values from -6 to 6
- keys: bfloat16 [16384, 2048], P(('grp', 'sp'), 'tp'), parts along dimension 0, may hold values from -6 to 6
- values: bfloat16 [16384, 2048], P(('grp', 'sp'), 'tp'), parts along dimension 0, may hold values from -8 to 8
- offsets: float32 [16], P('tp'), as said below
- residual: bfloat16 [16384, 4096], P(('grp', 'sp', 'tp')), parts along dimension 0, may hold values from -6 to 6
- out_weight: bfloat16 [2048, 4096], P('tp'), may hold values from -0.52734375 to 0.52734375
- gain_one: float32 [4096], replicated, may hold values from 0.1 to 1.9
- shift_one: float32 [4096], replicated, may hold values from -3 to 3
- gain_two: float32 [4096], replicated, may hold values from 0.1 to 1.9
- shift_two: float32 [4096], replicated, may hold values from -3 to 3
- group_prob: float32 [16384], P(('grp', 'sp', 'tp')), parts along dimension 0, may hold values from 0.2 to 1
- pair_logits: float32 [16384, 2], P(('grp', 'sp', 'tp')), parts along dimension 0, may hold values from -6 to 6
- routes: int32 [16384, 2], P(('grp', 'sp', 'tp')), parts along dimension 0, may hold values from 0 to 127, as said below
- w_gate: bfloat16 [128, 4096, 256], P(('sp', 'tp')), may hold values from -0.09375 to 0.09375
- w_up: bfloat16 [128, 4096, 256], P(('sp', 'tp')), may hold values from -0.09375 to 0.09375
- w_down: bfloat16 [128, 256, 4096], P(('sp', 'tp')), may hold values from -1.5 to 1.5
Outputs:
- layer_out: bfloat16 [16384, 4096], P(('grp', 'sp', 'tp')), parts along dimension 0
The draws below stay inside these ranges and needn't reach their ends.
There are 2 independent parts, one for each index of `grp`. The reference program is written for one: setup_inputs(seed, part) draws one part's arguments, and reference() takes and returns one part's arrays. A program takes and returns all parts, laid end to end along the dimension named above; an argument that names none is the same for every part. Nothing has to cross between parts.
Inputs may be any that keep to these rules, and one draw needn't show every extreme that they name: `routes`: both experts of a token are different and lie in one group of 32 consecutive experts. Of the tokens of one device (64 consecutive ones), at most 2 name any one expert; in every draw some experts are named exactly 2 times by the tokens of every device. `offsets`: each offset lies between 2.5 and ln(8192) - 0.3.
All inputs are finite; a program needn't handle non-finite values.
Results may differ from the reference program's by a relative error of at most 0.014.
Values may be sent and summed in bfloat16 or wider, within the bound.
No kernel may reach another device: no remote copies, remote signals or barrier semaphores. Data moves between devices by JAX's collectives and lax.ppermute only.
A program may use at most 128 MiB of HBM per device.

```python
import math
import jax
import jax.numpy as jnp
from jax import lax

D = 4096
HEADS = 16
HEAD_DIM = 128
FE = 256
GROUPS = 4
TOPK = 2
TOK_DEV = 256
TOKENS = 8192
ROWS = 64
EXPERTS = 128
EPG = 32
CAP = 2
N_SP = 32
N_TP = 4


def draw_offsets(key, part):
    upper = math.log(TOKENS) - 0.3
    slow_key, near_key, wide_key = jax.random.split(key, 3)
    slow = jax.random.uniform(slow_key, (HEADS,), jnp.float32) < 0.5
    near = jax.random.uniform(near_key, (HEADS,), jnp.float32, upper - 1.0, upper)
    wide = jnp.exp(jax.random.uniform(wide_key, (HEADS,), jnp.float32, math.log(2.5), math.log(upper - 1.0)))
    return jnp.where(slow, near, wide)


def draw_values(key, part):
    blocks = TOKENS // TOK_DEV
    width = HEADS * HEAD_DIM
    noise_key, mean_key = jax.random.split(jax.random.fold_in(key, 21))
    noise = jax.random.normal(noise_key, (blocks, TOK_DEV, width), jnp.float32)
    means = 2.0 * jax.random.normal(mean_key, (blocks, 1, width), jnp.float32)
    whole = jnp.clip(noise + means, -8.0, 8.0)
    return whole.reshape(TOKENS, width).astype(jnp.bfloat16)


def draw_routes(key, part):
    blocks = TOKENS // ROWS
    busy = jax.random.randint(jax.random.fold_in(key, 11), (), 0, GROUPS)

    def one_block(block_key):
        first_key, second_key, third_key, fourth_key = jax.random.split(block_key, 4)
        order = jax.random.permutation(first_key, ROWS)
        others = (busy + 1 + jax.random.randint(second_key, (ROWS,), 0, GROUPS - 1)) % GROUPS
        group = jnp.where(order < ROWS // 2, busy, others)
        onehot = (group[:, None] == jnp.arange(GROUPS)[None, :]).astype(jnp.int32)
        rank = jnp.sum((jnp.cumsum(onehot, axis=0) - onehot) * onehot, axis=1)
        start = jax.random.randint(third_key, (GROUPS,), 0, EPG)
        stride = jax.random.randint(fourth_key, (GROUPS,), 1, EPG)
        first = (start[group] + rank) % EPG
        second = (start[group] + rank + stride[group]) % EPG
        return jnp.stack([group * EPG + first, group * EPG + second], axis=1)
    block_keys = jax.random.split(jax.random.fold_in(key, 12), blocks)
    return jax.vmap(one_block)(block_keys).reshape(TOKENS, TOPK).astype(jnp.int32)


def shard_levels(own_key, extent, cuts, low, top_value):
    level = 1.0
    for dim, blocks in cuts:
        heights = jax.random.uniform(jax.random.fold_in(jax.random.fold_in(own_key, 6), dim), (blocks,), jnp.float32, low / len(cuts), top_value / len(cuts))
        level = level * jnp.repeat(jnp.exp(heights), extent[dim] // blocks).reshape((-1,) + (1,) * (len(extent) - 1 - dim))
    return level


def bell_draw(stream_key, shape, spread, reach, cuts=(), kind=jnp.bfloat16):
    loudness = shard_levels(stream_key, shape, cuts, -0.22, 0.18) if cuts else 1.0
    values = jax.random.normal(stream_key, shape, jnp.float32) * spread * loudness
    return jnp.minimum(jnp.maximum(values, -reach), reach).astype(kind)


def setup_inputs(seed: int = 0, part: int = 0) -> dict:
    key_list = jax.random.split(jax.random.key(seed), 17)
    own_keys = jax.random.split(jax.random.fold_in(key_list[16], part), 17)
    queries = bell_draw(own_keys[0], (TOKENS, HEADS * HEAD_DIM), 1.0, 6.0, ((0, 32), (1, 4)))
    keys = bell_draw(own_keys[1], (TOKENS, HEADS * HEAD_DIM), 1.0, 6.0, ((0, 32), (1, 4)))
    values = draw_values(jax.random.fold_in(jax.random.fold_in(key_list[16], part), 71), part)
    offsets = draw_offsets(jax.random.fold_in(key_list[16], 71), part)
    residual = bell_draw(own_keys[4], (TOKENS, D), 1.0, 6.0, ((0, 128),))
    out_weight = bell_draw(key_list[5], (HEADS * HEAD_DIM, D), (4.0 / (HEADS * HEAD_DIM) ** 0.5), 0.52734375, ((0, 4),))
    gain_one = jnp.clip(1.0 + 0.18 * jax.random.normal(key_list[6], (D,), jnp.float32), 0.1, 1.9)
    shift_one = bell_draw(key_list[7], (D,), 0.5, 3.0, (), jnp.float32)
    gain_two = jnp.clip(1.0 + 0.18 * jax.random.normal(key_list[8], (D,), jnp.float32), 0.1, 1.9)
    shift_two = bell_draw(key_list[9], (D,), 0.5, 3.0, (), jnp.float32)
    group_prob = jnp.clip(0.2 + 0.8 * jax.random.uniform(own_keys[10], (TOKENS,), jnp.float32) ** shard_levels(own_keys[10], (TOKENS,), ((0, 128),), -0.2, 0.2), 0.2, 1.0)
    pair_logits = bell_draw(own_keys[11], (TOKENS, TOPK), 1.5, 6.0, ((0, 128),), jnp.float32)
    routes = draw_routes(jax.random.fold_in(jax.random.fold_in(key_list[16], part), 71), part)
    w_gate = bell_draw(key_list[13], (EXPERTS, D, FE), D ** -0.5, 0.09375, ((0, 128),))
    w_up = bell_draw(key_list[14], (EXPERTS, D, FE), D ** -0.5, 0.09375, ((0, 128),))
    w_down = bell_draw(key_list[15], (EXPERTS, FE, D), (4.0 / FE ** 0.5), 1.5, ((0, 128),))
    return dict(queries=queries, keys=keys, values=values, offsets=offsets, residual=residual, out_weight=out_weight, gain_one=gain_one, shift_one=shift_one, gain_two=gain_two, shift_two=shift_two, group_prob=group_prob, pair_logits=pair_logits, routes=routes, w_gate=w_gate, w_up=w_up, w_down=w_down)


residual_scale = 8.0 ** 0.25
norm_eps = 1e-05

def layer_norm(rows, gain, shift):
    mean = lax.optimization_barrier(jnp.mean(rows, axis=-1, keepdims=True))
    centred = rows - mean
    variance = lax.optimization_barrier(jnp.mean(centred * centred, axis=-1, keepdims=True))
    return centred * lax.rsqrt(variance + norm_eps) * gain + shift

def slot_index(routes, expert_count, capacity):
    flat = routes.reshape(-1)
    onehot = (flat[:, None] == jnp.arange(expert_count, dtype=jnp.int32)[None, :]).astype(jnp.int32)
    earlier = jnp.cumsum(onehot, axis=0) - onehot
    rank = lax.optimization_barrier(jnp.sum(earlier * onehot, axis=1))
    return (flat * capacity + rank).astype(jnp.int32)

def attend(queries, keys, values, offsets):
    head_count = offsets.shape[0]
    query_heads = queries.reshape(TOKENS, head_count, HEAD_DIM)
    key_heads = keys.reshape(TOKENS, head_count, HEAD_DIM).astype(jnp.float32)
    value_heads = values.reshape(TOKENS, head_count, HEAD_DIM).astype(jnp.float32)
    key_pos = jnp.arange(TOKENS, dtype=jnp.int32)

    def block(index):
        start = (index * TOK_DEV).astype(jnp.int32)
        query_block = lax.dynamic_slice_in_dim(query_heads, start, TOK_DEV, 0).astype(jnp.float32)
        score = jnp.einsum('qhd,khd->hqk', query_block, key_heads) * HEAD_DIM ** (-0.5) - offsets[:, None, None]
        query_pos = start + jnp.arange(TOK_DEV, dtype=jnp.int32)
        strict = key_pos[None, :] < query_pos[:, None]
        keep = jnp.where(strict, jax.nn.log_sigmoid(-score), 0.0)
        later = lax.cumsum(keep, axis=2, reverse=True) - keep
        weight = jnp.where(strict, jnp.exp(jax.nn.log_sigmoid(score) + later), 0.0).astype(jnp.bfloat16)
        weight = lax.optimization_barrier(weight).astype(jnp.float32)
        return jnp.einsum('hqk,khd->qhd', weight, value_heads).astype(jnp.bfloat16)
    out = lax.map(block, jnp.arange(N_SP, dtype=jnp.int32))
    return out.reshape(TOKENS, head_count * HEAD_DIM)

def expert_rows(operands):
    rows, gate_w, up_w, down_w = operands
    gate = jnp.dot(rows, gate_w, preferred_element_type=jnp.float32)
    upper = jnp.dot(rows, up_w, preferred_element_type=jnp.float32)
    hidden = (jax.nn.silu(gate) * upper).astype(jnp.bfloat16)
    return jnp.dot(hidden, down_w, preferred_element_type=jnp.float32).astype(jnp.bfloat16)

def reference(queries, keys, values, offsets, residual, out_weight, gain_one, shift_one, gain_two, shift_two, group_prob, pair_logits, routes, w_gate, w_up, w_down):
    attended = attend(queries, keys, values, offsets)
    span = HEADS * HEAD_DIM // N_TP
    mixed = jnp.zeros((TOKENS, D), jnp.float32)
    for member in range(N_TP):
        partial_sum = jnp.dot(attended[:, member * span:(member + 1) * span], out_weight[member * span:(member + 1) * span], preferred_element_type=jnp.float32)
        partial_sum = lax.optimization_barrier(partial_sum.astype(jnp.bfloat16))
        mixed = mixed + partial_sum.astype(jnp.float32)
    normed = layer_norm(residual_scale * residual.astype(jnp.float32) + mixed, gain_one, shift_one).astype(jnp.bfloat16)
    sources = TOKENS // ROWS
    src_rows = normed.reshape(sources, ROWS, D)
    slots = jax.vmap(lambda part_routes: slot_index(part_routes, EXPERTS, CAP))(routes.reshape(sources, ROWS, TOPK))

    def fill(rows, slot):
        return jnp.zeros((EXPERTS * CAP, D), jnp.bfloat16).at[slot].set(jnp.repeat(rows, TOPK, axis=0))
    buffers = jax.vmap(fill)(src_rows, slots)
    per_expert = jnp.swapaxes(buffers.reshape(sources, EXPERTS, CAP, D), 0, 1).reshape(EXPERTS, sources * CAP, D)
    outputs = lax.map(expert_rows, (per_expert, w_gate, w_up, w_down))
    outputs = jnp.swapaxes(outputs.reshape(EXPERTS, sources, CAP, D), 0, 1).reshape(sources, EXPERTS * CAP, D)
    picked = jax.vmap(lambda rows, slot: rows[slot])(outputs, slots).reshape(TOKENS, TOPK, D)
    difference = pair_logits[:, 0] - pair_logits[:, 1]
    pair_weight = jnp.stack([jax.nn.sigmoid(difference), jax.nn.sigmoid(-difference)], axis=1)
    route_weight = group_prob[:, None] * pair_weight
    moe = lax.optimization_barrier(jnp.sum(route_weight[:, :, None] * picked.astype(jnp.float32), axis=1))
    return layer_norm(residual_scale * normed.astype(jnp.float32) + moe, gain_two, shift_two).astype(jnp.bfloat16)
```

```python
import functools
import jax
import jax.numpy as jnp
from jax import lax
from jax.experimental import pallas as pl
from jax.experimental.pallas import tpu as pltpu
from jax.sharding import PartitionSpec as P

HEAD_DIM = 128
GROUPS = 4
TOPK = 2


residual_scale = 8.0**0.25
norm_eps = 1e-05


LOG2E = 1.4426950408889634
def attn_body(where_ref, off_ref, q_ref, kv_ref, o_ref, acc_ref, carry_ref, *, heads, span, per_step, lo):
    step = pl.program_id(0)
    own = where_ref[0]
    top_step = own // per_step
    rows = q_ref.shape[0]
    scale = HEAD_DIM ** (-0.5) * LOG2E
    from_s = lax.broadcasted_iota(jnp.int32, (span, span), 0)
    to_s = lax.broadcasted_iota(jnp.int32, (span, span), 1)
    later = (from_s >= to_s).astype(jnp.float32).astype(jnp.bfloat16)
    both = jnp.concatenate([later, later], axis=0) if lo else later
    shift = to_s - from_s

    def blocks(masked):
        first = own - top_step * per_step
        for h in range(heads):
            cols = slice(h * HEAD_DIM, (h + 1) * HEAD_DIM)
            q = q_ref[:, cols]
            carry = carry_ref[:, cols][:, :1]
            acc = acc_ref[:, cols]
            for b in reversed(range(per_step)):
                k = kv_ref[b * span:(b + 1) * span, 2 * h * HEAD_DIM:(2 * h + 1) * HEAD_DIM]
                v = kv_ref[b * span:(b + 1) * span, (2 * h + 1) * HEAD_DIM:(2 * h + 2) * HEAD_DIM]
                s = lax.dot_general(q, k, (((1,), (1,)), ((), ())), preferred_element_type=jnp.float32)
                y = s * scale - off_ref[h] * LOG2E
                soft = jnp.maximum(y, jnp.log(1.0 + jnp.exp2(jnp.minimum(y, 126.0))) * LOG2E)
                if masked:
                    strict = shift < (first - b) * span
                    soft = jnp.where(strict, soft, 0.0)
                high = soft.astype(jnp.bfloat16)
                if lo:
                    low = (soft - high.astype(jnp.float32)).astype(jnp.bfloat16)
                    high = jnp.concatenate([high, low], axis=1)
                sums = jnp.dot(high, both, preferred_element_type=jnp.float32)
                weight = jnp.exp2(y - carry - sums)
                if masked:
                    weight = jnp.where(strict, weight, 0.0)
                carry = carry + sums[:, :1]
                acc = acc + jnp.dot(weight.astype(jnp.bfloat16), v, preferred_element_type=jnp.float32)
            carry_ref[:, cols] = jnp.broadcast_to(carry, (rows, HEAD_DIM))
            acc_ref[:, cols] = acc

    @pl.when(step == 0)
    def _():
        acc_ref[...] = jnp.zeros_like(acc_ref)
        carry_ref[...] = jnp.zeros_like(carry_ref)
        blocks(True)

    @pl.when((step > 0) & (step <= top_step))
    def _():
        blocks(False)

    @pl.when(step == pl.num_programs(0) - 1)
    def _():
        o_ref[...] = acc_ref[...].astype(jnp.bfloat16)

def attend(own, offsets, q, kv, heads, per_step=4, lo=False):
    rows = q.shape[0]
    span = rows
    blocks = kv.shape[0] // span
    w = heads * HEAD_DIM
    body = functools.partial(attn_body, heads=heads, span=span, per_step=per_step, lo=lo)
    return pl.pallas_call(
        body,
        grid_spec=pltpu.PrefetchScalarGridSpec(
            num_scalar_prefetch=2,
            grid=(blocks // per_step,),
            in_specs=[pl.BlockSpec((rows, w), lambda n, at, off: (0, 0)),
                      pl.BlockSpec((per_step * span, 2 * w), lambda n, at, off: (jnp.maximum(at[0] // per_step - n, 0), 0))],
            out_specs=pl.BlockSpec((rows, w), lambda n, at, off: (0, 0)),
            scratch_shapes=[pltpu.VMEM((rows, w), jnp.float32), pltpu.VMEM((rows, w), jnp.float32)],
        ),
        out_shape=jax.ShapeDtypeStruct((rows, w), jnp.bfloat16),
        name="attend",
    )(own, offsets, q, kv)


def cut_along(value, dim, peers):
    before, after = (value.shape[:dim], value.shape[dim + 1 :])
    return jnp.moveaxis(value.reshape(*before, peers, -1, *after), dim, 0)


def sent_and_summed(value, axis, dim):
    peers = lax.axis_size(axis)
    tiles = lax.all_to_all(cut_along(value, dim, peers), axis, 0, 0, tiled=True)
    return jnp.sum(tiles.astype(jnp.float32), axis=0)


def layer_norm(rows, gain, shift):
    mean = jnp.mean(rows, axis=-1, keepdims=True)
    centred = rows - mean
    variance = jnp.mean(centred * centred, axis=-1, keepdims=True)
    return centred * lax.rsqrt(variance + norm_eps) * gain + shift


def slot_index(routes, expert_count, capacity):
    flat = routes.reshape(-1)
    onehot = (flat[:, None] == jnp.arange(expert_count, dtype=jnp.int32)[None, :]).astype(jnp.int32)
    earlier = jnp.cumsum(onehot, axis=0) - onehot
    rank = jnp.sum(earlier * onehot, axis=1)
    return flat * capacity + rank


def expert_rows(rows, gate_w, up_w, down_w):
    gate = jnp.dot(rows, gate_w, preferred_element_type=jnp.float32)
    upper = jnp.dot(rows, up_w, preferred_element_type=jnp.float32)
    hidden = (jax.nn.silu(gate) * upper).astype(jnp.bfloat16)
    return jnp.dot(hidden, down_w, preferred_element_type=jnp.float32).astype(jnp.bfloat16)


def per_device(
    queries,
    keys,
    values,
    offsets,
    residual,
    out_weight,
    gain_one,
    shift_one,
    gain_two,
    shift_two,
    group_prob,
    pair_logits,
    routes,
    w_gate,
    w_up,
    w_down,
):
    row_count = queries.shape[0]
    head_count = offsets.shape[0]
    own = lax.axis_index("sp").astype(jnp.int32).reshape(1)
    pairs = []
    for h in range(head_count):
        cols = slice(h * HEAD_DIM, (h + 1) * HEAD_DIM)
        pairs += [keys[:, cols], values[:, cols]]
    every = lax.all_gather(jnp.concatenate(pairs, axis=1), "sp", axis=0, tiled=True)
    attended_rows = attend(own, offsets, queries, every, head_count)
    local_rows = residual.shape[0]
    mixed = sent_and_summed(
        jnp.dot(attended_rows, out_weight, preferred_element_type=jnp.float32).astype(jnp.bfloat16),
        "tp",
        0,
    )
    normed = layer_norm(
        residual_scale * residual.astype(jnp.float32) + mixed, gain_one, shift_one
    ).astype(jnp.bfloat16)
    width = normed.shape[1]
    expert_count = lax.axis_size("sp") * lax.axis_size("tp")
    capacity = local_rows // (expert_count // GROUPS)
    slots = slot_index(routes, expert_count, capacity)
    buffer = (
        jnp.zeros((expert_count * capacity, width), jnp.bfloat16)
        .at[slots]
        .set(jnp.repeat(normed, TOPK, axis=0))
    )
    arrived = lax.all_to_all(
        buffer.reshape(expert_count, capacity, width),
        ("sp", "tp"),
        split_axis=0,
        concat_axis=0,
        tiled=True,
    )
    result = expert_rows(arrived.reshape(-1, width), w_gate[0], w_up[0], w_down[0]).reshape(
        expert_count, capacity, width
    )
    returned = lax.all_to_all(result, ("sp", "tp"), split_axis=0, concat_axis=0, tiled=True)
    picked = returned.reshape(-1, width)[slots].reshape(local_rows, TOPK, width)
    difference = pair_logits[:, 0] - pair_logits[:, 1]
    pair_weight = jnp.stack([jax.nn.sigmoid(difference), jax.nn.sigmoid(-difference)], axis=1)
    route_weight = group_prob[:, None] * pair_weight
    moe = jnp.sum(route_weight[:, :, None] * picked.astype(jnp.float32), axis=1)
    return layer_norm(
        residual_scale * normed.astype(jnp.float32) + moe, gain_two, shift_two
    ).astype(jnp.bfloat16)


def solution(mesh):
    return jax.shard_map(
        per_device,
        mesh=mesh,
        in_specs=(
            P(("grp", "sp"), "tp"),
            P(("grp", "sp"), "tp"),
            P(("grp", "sp"), "tp"),
            P("tp"),
            P(("grp", "sp", "tp"), None),
            P("tp", None),
            P(),
            P(),
            P(),
            P(),
            P(("grp", "sp", "tp")),
            P(("grp", "sp", "tp"), None),
            P(("grp", "sp", "tp"), None),
            P(("sp", "tp"), None, None),
            P(("sp", "tp"), None, None),
            P(("sp", "tp"), None, None),
        ),
        out_specs=P(("grp", "sp", "tp"), None),
        check_vma=False,
    )
```

```python
import functools
import jax
import jax.numpy as jnp
from jax import lax
from jax.experimental import pallas as pl
from jax.experimental.pallas import tpu as pltpu
from jax.sharding import PartitionSpec as P

HEAD_DIM = 128
GROUPS = 4
TOPK = 2


residual_scale = 8.0**0.25
norm_eps = 1e-05


LOG2E = 1.4426950408889634
EXP_CAP = 126.0


def key_tile(q, k, v, offset, later, carry, strict):
    score = lax.dot_general(q, k, (((1,), (1,)), ((), ())), preferred_element_type=jnp.float32)
    y = score * (HEAD_DIM ** (-0.5) * LOG2E) - offset * LOG2E
    soft = jnp.maximum(y, jnp.log(1.0 + jnp.exp2(jnp.minimum(y, EXP_CAP))) * LOG2E)
    if strict is not None:
        soft = jnp.where(strict, soft, 0.0)
    sums = jnp.dot(soft.astype(jnp.bfloat16), later, preferred_element_type=jnp.float32)
    weight = jnp.exp2(y - carry - sums)
    if strict is not None:
        weight = jnp.where(strict, weight, 0.0)
    part = jnp.dot(weight.astype(jnp.bfloat16), v, preferred_element_type=jnp.float32)
    return part, carry + sums[:, :1]


def head_cols(h):
    return pl.ds(pl.multiple_of(h * HEAD_DIM, HEAD_DIM), HEAD_DIM)


def each_head(q_ref, body):
    def one(h, unused):
        body(h, head_cols(h))
        return unused

    lax.fori_loop(0, q_ref.shape[1] // HEAD_DIM, one, 0)


def chunk_part(off_ref, q_ref, k_ref, v_ref, h, carry, masked):
    rows, span = q_ref.shape[0], 256
    cols = head_cols(h)
    from_s = lax.broadcasted_iota(jnp.int32, (span, span), 0)
    to_s = lax.broadcasted_iota(jnp.int32, (span, span), 1)
    later = (from_s >= to_s).astype(jnp.float32).astype(jnp.bfloat16)
    q = q_ref[:, cols]
    total = None
    for start in reversed(range(0, k_ref.shape[0], span)):
        strict = None
        if masked:
            at_q = lax.broadcasted_iota(jnp.int32, (rows, span), 0)
            at_k = lax.broadcasted_iota(jnp.int32, (rows, span), 1) + start
            strict = at_k < at_q
        part, carry = key_tile(
            q, k_ref[start:start + span, cols], v_ref[start:start + span, cols],
            off_ref[h], later, carry, strict,
        )
        total = part if total is None else total + part
    return total, carry


def wide(column):
    return jnp.broadcast_to(column, (column.shape[0], HEAD_DIM))


def own_chunk_body(off_ref, q_ref, k_ref, v_ref, near_ref, carry_ref):
    def one(h, cols):
        zero = jnp.zeros((q_ref.shape[0], 1), jnp.float32)
        part, carry = chunk_part(off_ref, q_ref, k_ref, v_ref, h, zero, True)
        near_ref[:, cols] = part
        carry_ref[:, cols] = wide(carry)

    each_head(q_ref, one)


def near_update(off_ref, q_ref, k_ref, v_ref, near_in, carry_in, near_ref, carry_ref):
    def one(h, cols):
        part, carry = chunk_part(off_ref, q_ref, k_ref, v_ref, h, carry_in[:, cols][:, :1], False)
        near_ref[:, cols] = near_in[:, cols] + part
        carry_ref[:, cols] = wide(carry)

    each_head(q_ref, one)


def far_update(off_ref, q_ref, k_ref, v_ref, far_in, far_ref):
    def one(h, cols):
        zero = jnp.zeros((q_ref.shape[0], 1), jnp.float32)
        part, carry = chunk_part(off_ref, q_ref, k_ref, v_ref, h, zero, False)
        far_ref[:, cols] = part + far_in[:, cols] * jnp.exp2(-carry)

    each_head(q_ref, one)


def hop_body(hop, places, first, place_ref, off_ref, q_ref, kn, vn, kf, vf, near_in, carry_in, *rest):
    if first:
        near_ref, carry_ref, far_ref = rest
    else:
        far_in, near_ref, carry_ref, far_ref = rest

    @pl.when(place_ref[0] >= hop)
    def _():
        near_update(off_ref, q_ref, kn, vn, near_in, carry_in, near_ref, carry_ref)

    @pl.when(place_ref[0] < hop)
    def _():
        near_ref[...] = near_in[...]
        carry_ref[...] = carry_in[...]

    if first:
        far_ref[...] = jnp.zeros_like(far_ref)
        far_in = far_ref

    @pl.when(place_ref[0] + hop >= places)
    def _():
        far_update(off_ref, q_ref, kf, vf, far_in, far_ref)

    if not first:
        @pl.when(place_ref[0] + hop < places)
        def _():
            far_ref[...] = far_in[...]


def last_body(hop, place_ref, off_ref, q_ref, kn, vn, near_in, carry_in, far_in, out_ref, near_ref, carry_ref):
    near_ref[...] = near_in[...]
    carry_ref[...] = carry_in[...]

    @pl.when(place_ref[0] >= hop)
    def _():
        near_update(off_ref, q_ref, kn, vn, near_in, carry_in, near_ref, carry_ref)

    out_ref[...] = (near_ref[...] + jnp.exp2(-carry_ref[...]) * far_in[...]).astype(jnp.bfloat16)


def run_local(body, name, scalars, arrays, outs, scratch=(), chunks=1):
    smem = pl.BlockSpec(memory_space=pltpu.SMEM)
    vmem = pl.BlockSpec(memory_space=pltpu.VMEM)
    rows, width = arrays[0].shape
    tiles = chunks * rows * arrays[1].shape[0] * (width // HEAD_DIM)
    return pl.pallas_call(
        body,
        in_specs=[smem] * len(scalars) + [vmem] * len(arrays),
        out_specs=jax.tree.map(lambda _: vmem, outs),
        out_shape=outs,
        scratch_shapes=list(scratch),
        cost_estimate=pl.CostEstimate(flops=tiles * 2 * 2 * (HEAD_DIM + HEAD_DIM), transcendentals=3 * tiles, bytes_accessed=4 * rows * width),
        name=name,
    )(*scalars, *arrays)


def ring_attend(queries, keys, values, offsets):
    devices = lax.axis_size("sp")
    places = devices // 2
    me = lax.axis_index("sp").astype(jnp.int32)
    core, place = me % 2, me // 2
    heads = offsets.shape[0] // 2
    half = heads * HEAD_DIM
    mate = [(i, i ^ 1) for i in range(devices)]

    def split(a):
        low, high = a[:, :half], a[:, half:]
        return jnp.where(core == 0, low, high), jnp.where(core == 0, high, low)

    def traded(a):
        kept, given = split(a)
        got = lax.ppermute(given, "sp", mate)
        return jnp.concatenate([jnp.where(core == 0, kept, got), jnp.where(core == 0, got, kept)], axis=0)

    k, v, q = traded(keys), traded(values), traded(queries)
    off = jnp.where(core == 0, offsets[:heads], offsets[heads:])
    state = jax.ShapeDtypeStruct((q.shape[0], half), jnp.float32)
    up = [(i, (i + 2) % devices) for i in range(devices)]
    down = [(i, (i - 2) % devices) for i in range(devices)]
    near, carry = run_local(own_chunk_body, "own_chunk", (off,), (q, k, v), (state, state))
    near_hops = places // 2
    far_hops = places - 1 - near_hops
    place = place.reshape(1)
    near_now = tuple(lax.ppermute(a, "sp", up) for a in (k, v))
    far_now = tuple(lax.ppermute(a, "sp", down) for a in (k, v))
    far = None
    for hop in range(1, near_hops + 1):
        near_next, far_next = [], []
        for i in range(2):
            if hop < near_hops:
                tied, near = lax.optimization_barrier((near_now[i], near))
                near_next.append(lax.ppermute(tied, "sp", up))
            if hop < far_hops:
                tied, near = lax.optimization_barrier((far_now[i], near))
                far_next.append(lax.ppermute(tied, "sp", down))
        if hop <= far_hops:
            first = far is None
            near, carry, far = run_local(
                functools.partial(hop_body, hop, places, first), "hop",
                (place, off), (q, *near_now, *far_now, near, carry) + (() if first else (far,)),
                (state, state, state), chunks=2,
            )
        else:
            out = jax.ShapeDtypeStruct(q.shape, jnp.bfloat16)
            attended = run_local(
                functools.partial(last_body, hop), "last_hop",
                (place, off), (q, *near_now, near, carry, far), out,
                scratch=(pltpu.VMEM(state.shape, jnp.float32), pltpu.VMEM(state.shape, jnp.float32)),
            )
        near_now, far_now = near_next, far_next
    rows = queries.shape[0]
    first_rows, second_rows = attended[:rows], attended[rows:]
    kept = jnp.where(core == 0, first_rows, second_rows)
    got = lax.ppermute(jnp.where(core == 0, second_rows, first_rows), "sp", mate)
    return jnp.where(core == 0, jnp.concatenate([kept, got], axis=1), jnp.concatenate([got, kept], axis=1))


def cut_along(value, dim, peers):
    before, after = (value.shape[:dim], value.shape[dim + 1 :])
    return jnp.moveaxis(value.reshape(*before, peers, -1, *after), dim, 0)


def sent_and_summed(value, axis, dim):
    peers = lax.axis_size(axis)
    tiles = lax.all_to_all(cut_along(value, dim, peers), axis, 0, 0, tiled=True)
    return jnp.sum(tiles.astype(jnp.float32), axis=0)


def layer_norm(rows, gain, shift):
    mean = jnp.mean(rows, axis=-1, keepdims=True)
    centred = rows - mean
    variance = jnp.mean(centred * centred, axis=-1, keepdims=True)
    return centred * lax.rsqrt(variance + norm_eps) * gain + shift


def slot_index(routes, expert_count, capacity):
    flat = routes.reshape(-1)
    onehot = (flat[:, None] == jnp.arange(expert_count, dtype=jnp.int32)[None, :]).astype(jnp.int32)
    earlier = jnp.cumsum(onehot, axis=0) - onehot
    rank = jnp.sum(earlier * onehot, axis=1)
    return flat * capacity + rank


def expert_rows(rows, gate_w, up_w, down_w):
    gate = jnp.dot(rows, gate_w, preferred_element_type=jnp.float32)
    upper = jnp.dot(rows, up_w, preferred_element_type=jnp.float32)
    hidden = (jax.nn.silu(gate) * upper).astype(jnp.bfloat16)
    return jnp.dot(hidden, down_w, preferred_element_type=jnp.float32).astype(jnp.bfloat16)


def per_device(
    queries,
    keys,
    values,
    offsets,
    residual,
    out_weight,
    gain_one,
    shift_one,
    gain_two,
    shift_two,
    group_prob,
    pair_logits,
    routes,
    w_gate,
    w_up,
    w_down,
):
    attended_rows = ring_attend(queries, keys, values, offsets)
    local_rows = residual.shape[0]
    mixed = sent_and_summed(
        jnp.dot(attended_rows, out_weight, preferred_element_type=jnp.float32).astype(jnp.bfloat16),
        "tp",
        0,
    )
    normed = layer_norm(
        residual_scale * residual.astype(jnp.float32) + mixed, gain_one, shift_one
    ).astype(jnp.bfloat16)
    width = normed.shape[1]
    expert_count = lax.axis_size("sp") * lax.axis_size("tp")
    capacity = local_rows // (expert_count // GROUPS)
    slots = slot_index(routes, expert_count, capacity)
    buffer = (
        jnp.zeros((expert_count * capacity, width), jnp.bfloat16)
        .at[slots]
        .set(jnp.repeat(normed, TOPK, axis=0))
    )
    arrived = lax.all_to_all(
        buffer.reshape(expert_count, capacity, width),
        ("sp", "tp"),
        split_axis=0,
        concat_axis=0,
        tiled=True,
    )
    result = expert_rows(arrived.reshape(-1, width), w_gate[0], w_up[0], w_down[0]).reshape(
        expert_count, capacity, width
    )
    returned = lax.all_to_all(result, ("sp", "tp"), split_axis=0, concat_axis=0, tiled=True)
    picked = returned.reshape(-1, width)[slots].reshape(local_rows, TOPK, width)
    difference = pair_logits[:, 0] - pair_logits[:, 1]
    pair_weight = jnp.stack([jax.nn.sigmoid(difference), jax.nn.sigmoid(-difference)], axis=1)
    route_weight = group_prob[:, None] * pair_weight
    moe = jnp.sum(route_weight[:, :, None] * picked.astype(jnp.float32), axis=1)
    return layer_norm(
        residual_scale * normed.astype(jnp.float32) + moe, gain_two, shift_two
    ).astype(jnp.bfloat16)


def solution(mesh):
    return jax.shard_map(
        per_device,
        mesh=mesh,
        in_specs=(
            P(("grp", "sp"), "tp"),
            P(("grp", "sp"), "tp"),
            P(("grp", "sp"), "tp"),
            P("tp"),
            P(("grp", "sp", "tp"), None),
            P("tp", None),
            P(),
            P(),
            P(),
            P(),
            P(("grp", "sp", "tp")),
            P(("grp", "sp", "tp"), None),
            P(("grp", "sp", "tp"), None),
            P(("sp", "tp"), None, None),
            P(("sp", "tp"), None, None),
            P(("sp", "tp"), None, None),
        ),
        out_specs=P(("grp", "sp", "tp"), None),
        check_vma=False,
    )
```

```python
import functools
import jax
import jax.numpy as jnp
from jax import lax
from jax.experimental import pallas as pl
from jax.experimental.pallas import tpu as pltpu
from jax.sharding import PartitionSpec as P

HEAD_DIM = 128
GROUPS = 4
TOPK = 2


residual_scale = 8.0**0.25
norm_eps = 1e-05


LOG2E = 1.4426950408889634
EXP_CAP = 126.0


def key_tile(q, k, v, offset, later, carry, strict):
    score = lax.dot_general(q, k, (((1,), (1,)), ((), ())), preferred_element_type=jnp.float32)
    y = score * (HEAD_DIM ** (-0.5) * LOG2E) - offset * LOG2E
    soft = jnp.maximum(y, jnp.log(1.0 + jnp.exp2(jnp.minimum(y, EXP_CAP))) * LOG2E)
    if strict is not None:
        soft = jnp.where(strict, soft, 0.0)
    sums = jnp.dot(soft.astype(jnp.bfloat16), later, preferred_element_type=jnp.float32)
    weight = jnp.exp2(y - carry - sums)
    if strict is not None:
        weight = jnp.where(strict, weight, 0.0)
    part = jnp.dot(weight.astype(jnp.bfloat16), v, preferred_element_type=jnp.float32)
    return part, carry + sums[:, :1]


def head_cols(h):
    return pl.ds(pl.multiple_of(h * HEAD_DIM, HEAD_DIM), HEAD_DIM)


def each_head(q_ref, body):
    def one(h, unused):
        body(h, head_cols(h))
        return unused

    lax.fori_loop(0, q_ref.shape[1] // HEAD_DIM, one, 0)


def chunk_part(off_ref, q_ref, k_ref, v_ref, h, carry, masked):
    rows, span = q_ref.shape[0], 256
    cols = head_cols(h)
    from_s = lax.broadcasted_iota(jnp.int32, (span, span), 0)
    to_s = lax.broadcasted_iota(jnp.int32, (span, span), 1)
    later = (from_s >= to_s).astype(jnp.float32).astype(jnp.bfloat16)
    q = q_ref[:, cols]
    total = None
    for start in reversed(range(0, k_ref.shape[0], span)):
        strict = None
        if masked:
            at_q = lax.broadcasted_iota(jnp.int32, (rows, span), 0)
            at_k = lax.broadcasted_iota(jnp.int32, (rows, span), 1) + start
            strict = at_k < at_q
        part, carry = key_tile(
            q, k_ref[start:start + span, cols], v_ref[start:start + span, cols],
            off_ref[h], later, carry, strict,
        )
        total = part if total is None else total + part
    return total, carry


def wide(column):
    return jnp.broadcast_to(column, (column.shape[0], HEAD_DIM))


def own_chunk_body(off_ref, q_ref, k_ref, v_ref, near_ref, carry_ref):
    def one(h, cols):
        zero = jnp.zeros((q_ref.shape[0], 1), jnp.float32)
        part, carry = chunk_part(off_ref, q_ref, k_ref, v_ref, h, zero, True)
        near_ref[:, cols] = part
        carry_ref[:, cols] = wide(carry)

    each_head(q_ref, one)


def near_update(off_ref, q_ref, k_ref, v_ref, near_in, carry_in, near_ref, carry_ref):
    def one(h, cols):
        part, carry = chunk_part(off_ref, q_ref, k_ref, v_ref, h, carry_in[:, cols][:, :1], False)
        near_ref[:, cols] = near_in[:, cols] + part
        carry_ref[:, cols] = wide(carry)

    each_head(q_ref, one)


def far_update(off_ref, q_ref, k_ref, v_ref, far_in, far_ref):
    def one(h, cols):
        zero = jnp.zeros((q_ref.shape[0], 1), jnp.float32)
        part, carry = chunk_part(off_ref, q_ref, k_ref, v_ref, h, zero, False)
        far_ref[:, cols] = part + far_in[:, cols] * jnp.exp2(-carry)

    each_head(q_ref, one)


def hop_body(hop, places, first, place_ref, off_ref, q_ref, kn, vn, kf, vf, near_in, carry_in, *rest):
    if first:
        near_ref, carry_ref, far_ref = rest
    else:
        far_in, near_ref, carry_ref, far_ref = rest

    @pl.when(place_ref[0] >= hop)
    def _():
        near_update(off_ref, q_ref, kn, vn, near_in, carry_in, near_ref, carry_ref)

    @pl.when(place_ref[0] < hop)
    def _():
        near_ref[...] = near_in[...]
        carry_ref[...] = carry_in[...]

    if first:
        far_ref[...] = jnp.zeros_like(far_ref)
        far_in = far_ref

    @pl.when(place_ref[0] + hop >= places)
    def _():
        far_update(off_ref, q_ref, kf, vf, far_in, far_ref)

    if not first:
        @pl.when(place_ref[0] + hop < places)
        def _():
            far_ref[...] = far_in[...]


def last_body(hop, place_ref, off_ref, q_ref, kn, vn, near_in, carry_in, far_in, out_ref, near_ref, carry_ref):
    near_ref[...] = near_in[...]
    carry_ref[...] = carry_in[...]

    @pl.when(place_ref[0] >= hop)
    def _():
        near_update(off_ref, q_ref, kn, vn, near_in, carry_in, near_ref, carry_ref)

    out_ref[...] = (near_ref[...] + jnp.exp2(-carry_ref[...]) * far_in[...]).astype(jnp.bfloat16)


def run_local(body, name, scalars, arrays, outs, scratch=(), chunks=1):
    smem = pl.BlockSpec(memory_space=pltpu.SMEM)
    vmem = pl.BlockSpec(memory_space=pltpu.VMEM)
    rows, width = arrays[0].shape
    tiles = chunks * rows * arrays[1].shape[0] * (width // HEAD_DIM)
    return pl.pallas_call(
        body,
        in_specs=[smem] * len(scalars) + [vmem] * len(arrays),
        out_specs=jax.tree.map(lambda _: vmem, outs),
        out_shape=outs,
        scratch_shapes=list(scratch),
        cost_estimate=pl.CostEstimate(flops=tiles * 2 * 2 * (HEAD_DIM + HEAD_DIM), transcendentals=3 * tiles, bytes_accessed=4 * rows * width),
        name=name,
    )(*scalars, *arrays)


def ring_attend(queries, keys, values, offsets):
    devices = lax.axis_size("sp")
    places = devices // 2
    me = lax.axis_index("sp").astype(jnp.int32)
    core, place = me % 2, me // 2
    heads = offsets.shape[0] // 2
    half = heads * HEAD_DIM
    mate = [(i, i ^ 1) for i in range(devices)]

    def split(a):
        low, high = a[:, :half], a[:, half:]
        return jnp.where(core == 0, low, high), jnp.where(core == 0, high, low)

    def traded(a):
        kept, given = split(a)
        got = lax.ppermute(given, "sp", mate)
        return jnp.concatenate([jnp.where(core == 0, kept, got), jnp.where(core == 0, got, kept)], axis=0)

    k, v, q = traded(keys), traded(values), traded(queries)
    off = jnp.where(core == 0, offsets[:heads], offsets[heads:])
    state = jax.ShapeDtypeStruct((q.shape[0], half), jnp.float32)
    up = [(i, (i + 2) % devices) for i in range(devices)]
    down = [(i, (i - 2) % devices) for i in range(devices)]
    near, carry = run_local(own_chunk_body, "own_chunk", (off,), (q, k, v), (state, state))
    near_hops = places // 2
    far_hops = places - 1 - near_hops
    place = place.reshape(1)
    near_now = tuple(lax.ppermute(a, "sp", up) for a in (k, v))
    far_now = tuple(lax.ppermute(a, "sp", down) for a in (k, v))
    far = None
    for hop in range(1, near_hops + 1):
        near_next, far_next = [], []
        for i in range(2):
            if hop < near_hops:
                tied, near = lax.optimization_barrier((near_now[i], near))
                near_next.append(lax.ppermute(tied, "sp", up))
            if hop < far_hops:
                tied, near = lax.optimization_barrier((far_now[i], near))
                far_next.append(lax.ppermute(tied, "sp", down))
        if hop <= far_hops:
            first = far is None
            near, carry, far = run_local(
                functools.partial(hop_body, hop, places, first), "hop",
                (place, off), (q, *near_now, *far_now, near, carry) + (() if first else (far,)),
                (state, state, state), chunks=2,
            )
        else:
            out = jax.ShapeDtypeStruct(q.shape, jnp.bfloat16)
            attended = run_local(
                functools.partial(last_body, hop), "last_hop",
                (place, off), (q, *near_now, near, carry, far), out,
                scratch=(pltpu.VMEM(state.shape, jnp.float32), pltpu.VMEM(state.shape, jnp.float32)),
            )
        near_now, far_now = near_next, far_next
    rows = queries.shape[0]
    first_rows, second_rows = attended[:rows], attended[rows:]
    kept = jnp.where(core == 0, first_rows, second_rows)
    got = lax.ppermute(jnp.where(core == 0, second_rows, first_rows), "sp", mate)
    return jnp.where(core == 0, jnp.concatenate([kept, got], axis=1), jnp.concatenate([got, kept], axis=1))


def cut_along(value, dim, peers):
    before, after = (value.shape[:dim], value.shape[dim + 1 :])
    return jnp.moveaxis(value.reshape(*before, peers, -1, *after), dim, 0)


def sent_over(value, axis, dim):
    peers = lax.axis_size(axis)
    return lax.all_to_all(cut_along(value, dim, peers), axis, 0, 0, tiled=True)


def normalised(rows, gain, shift):
    mean = jnp.mean(rows, axis=-1, keepdims=True)
    centred = rows - mean
    variance = jnp.mean(centred * centred, axis=-1, keepdims=True)
    return centred * lax.rsqrt(variance + norm_eps) * gain + shift


def send_body(target_ref, tiles_ref, residual_ref, gain_ref, shift_ref, normed_ref, buffer_ref):
    mixed = tiles_ref[0].astype(jnp.float32)
    for member in range(1, tiles_ref.shape[0]):
        mixed = mixed + tiles_ref[member].astype(jnp.float32)
    rows = residual_scale * residual_ref[...].astype(jnp.float32) + mixed
    normed = normalised(rows, gain_ref[...], shift_ref[...]).astype(jnp.bfloat16)
    normed_ref[...] = normed
    width = buffer_ref.shape[1]
    pieces = jnp.concatenate(
        [normed[:, start:start + width] for start in range(0, normed.shape[1], width)], axis=0
    )
    first, second = target_ref[0:1, :], target_ref[1:2, :]
    block = 256

    def fill(n, unused):
        start = pl.multiple_of(n * block, block)
        at = lax.broadcasted_iota(jnp.int32, (block, pieces.shape[0]), 0) + start
        chosen = ((at == first) | (at == second)).astype(jnp.float32).astype(jnp.bfloat16)
        buffer_ref[pl.ds(start, block), :] = jnp.dot(
            chosen, pieces, preferred_element_type=jnp.float32
        ).astype(jnp.bfloat16)
        return unused

    lax.fori_loop(0, buffer_ref.shape[0] // block, fill, 0)


def receive_body(meta_ref, returned_ref, normed_ref, gain_ref, shift_ref, out_ref, one_ref, two_ref):
    count, width = meta_ref.shape[0], returned_ref.shape[1]
    first = meta_ref[:, 0:1].astype(jnp.int32)
    second = meta_ref[:, 1:2].astype(jnp.int32)
    block = 256
    one_ref[...] = jnp.zeros_like(one_ref)
    two_ref[...] = jnp.zeros_like(two_ref)

    def pick(n, unused):
        start = pl.multiple_of(n * block, block)
        at = lax.broadcasted_iota(jnp.int32, (count, block), 1) + start
        rows = returned_ref[pl.ds(start, block), :]
        for target, total_ref in ((first, one_ref), (second, two_ref)):
            chosen = (at == target).astype(jnp.float32).astype(jnp.bfloat16)
            total_ref[...] += jnp.dot(chosen, rows, preferred_element_type=jnp.float32)
        return unused

    lax.fori_loop(0, returned_ref.shape[0] // block, pick, 0)
    moe = meta_ref[:, 2:3] * one_ref[...] + meta_ref[:, 3:4] * two_ref[...]
    tokens = normed_ref.shape[0]
    moe = jnp.concatenate([moe[start:start + tokens] for start in range(0, count, tokens)], axis=1)
    rows = residual_scale * normed_ref[...].astype(jnp.float32) + moe
    out_ref[...] = normalised(rows, gain_ref[...], shift_ref[...]).astype(jnp.bfloat16)


def whole(body, name, arrays, outs, scratch=()):
    vmem = pl.BlockSpec(memory_space=pltpu.VMEM)
    return pl.pallas_call(
        body,
        in_specs=[vmem] * len(arrays),
        out_specs=jax.tree.map(lambda _: vmem, outs),
        out_shape=outs,
        scratch_shapes=list(scratch),
        name=name,
    )(*arrays)


def slot_index(routes, expert_count, capacity):
    flat = routes.reshape(-1)
    onehot = (flat[:, None] == jnp.arange(expert_count, dtype=jnp.int32)[None, :]).astype(jnp.int32)
    earlier = jnp.cumsum(onehot, axis=0) - onehot
    rank = jnp.sum(earlier * onehot, axis=1)
    return flat * capacity + rank


def expert_rows(rows, gate_w, up_w, down_w):
    gate = jnp.dot(rows, gate_w, preferred_element_type=jnp.float32)
    upper = jnp.dot(rows, up_w, preferred_element_type=jnp.float32)
    hidden = (jax.nn.silu(gate) * upper).astype(jnp.bfloat16)
    return jnp.dot(hidden, down_w, preferred_element_type=jnp.float32).astype(jnp.bfloat16)


def per_device(
    queries,
    keys,
    values,
    offsets,
    residual,
    out_weight,
    gain_one,
    shift_one,
    gain_two,
    shift_two,
    group_prob,
    pair_logits,
    routes,
    w_gate,
    w_up,
    w_down,
):
    attended_rows = ring_attend(queries, keys, values, offsets)
    local_rows = residual.shape[0]
    width = residual.shape[1]
    expert_count = lax.axis_size("sp") * lax.axis_size("tp")
    capacity = local_rows // (expert_count // GROUPS)
    slot_count = expert_count * capacity
    cuts = 16 // capacity
    piece = width // cuts
    slots = slot_index(routes, expert_count, capacity).reshape(local_rows, TOPK)
    cut = jnp.arange(cuts, dtype=jnp.int32)[None, :, None]
    targets = (slots.T[:, None, :] * cuts + cut).reshape(TOPK, cuts * local_rows)
    difference = pair_logits[:, 0] - pair_logits[:, 1]
    pair_weight = jnp.stack([jax.nn.sigmoid(difference), jax.nn.sigmoid(-difference)], axis=0)
    route_weight = jnp.tile(group_prob[None, :] * pair_weight, (1, cuts))
    meta = jnp.concatenate([targets.astype(jnp.float32), route_weight], axis=0).T
    tiles = sent_over(
        jnp.dot(attended_rows, out_weight, preferred_element_type=jnp.float32).astype(jnp.bfloat16),
        "tp",
        0,
    )
    buffer_shape = jax.ShapeDtypeStruct((slot_count * cuts, piece), jnp.bfloat16)
    rows_shape = jax.ShapeDtypeStruct((local_rows, width), jnp.bfloat16)
    normed, buffer = whole(
        send_body, "norm_and_place",
        (targets, tiles, residual, gain_one[None, :], shift_one[None, :]), (rows_shape, buffer_shape),
    )
    arrived = lax.all_to_all(buffer, ("sp", "tp"), split_axis=0, concat_axis=0, tiled=True)
    result = expert_rows(arrived.reshape(slot_count, width), w_gate[0], w_up[0], w_down[0])
    returned = lax.all_to_all(
        result.reshape(slot_count * cuts, piece), ("sp", "tp"), split_axis=0, concat_axis=0, tiled=True
    )
    picked = pltpu.VMEM((cuts * local_rows, piece), jnp.float32)
    return whole(
        receive_body, "pick_and_norm",
        (meta, returned, normed, gain_two[None, :], shift_two[None, :]), rows_shape, (picked, picked),
    )


def solution(mesh):
    return jax.shard_map(
        per_device,
        mesh=mesh,
        in_specs=(
            P(("grp", "sp"), "tp"),
            P(("grp", "sp"), "tp"),
            P(("grp", "sp"), "tp"),
            P("tp"),
            P(("grp", "sp", "tp"), None),
            P("tp", None),
            P(),
            P(),
            P(),
            P(),
            P(("grp", "sp", "tp")),
            P(("grp", "sp", "tp"), None),
            P(("grp", "sp", "tp"), None),
            P(("sp", "tp"), None, None),
            P(("sp", "tp"), None, None),
            P(("sp", "tp"), None, None),
        ),
        out_specs=P(("grp", "sp", "tp"), None),
        check_vma=False,
    )
```

```python
import functools
import jax
import jax.numpy as jnp
from jax import lax
from jax.experimental import pallas as pl
from jax.experimental.pallas import tpu as pltpu
from jax.sharding import PartitionSpec as P

HEAD_DIM = 128
GROUPS = 4
TOPK = 2


residual_scale = 8.0**0.25
norm_eps = 1e-05


LOG2E = 1.4426950408889634
EXP_CAP = 126.0


def key_tile(q, k, v, offset, later, carry, strict):
    score = lax.dot_general(q, k, (((1,), (1,)), ((), ())), preferred_element_type=jnp.float32)
    y = score * (HEAD_DIM ** (-0.5) * LOG2E) - offset * LOG2E
    soft = jnp.maximum(y, jnp.log(1.0 + jnp.exp2(jnp.minimum(y, EXP_CAP))) * LOG2E)
    if strict is not None:
        soft = jnp.where(strict, soft, 0.0)
    sums = jnp.dot(soft.astype(jnp.bfloat16), later, preferred_element_type=jnp.float32)
    weight = jnp.exp2(y - carry - sums)
    if strict is not None:
        weight = jnp.where(strict, weight, 0.0)
    part = jnp.dot(weight.astype(jnp.bfloat16), v, preferred_element_type=jnp.float32)
    return part, carry + sums[:, :1]


def head_cols(h):
    return pl.ds(pl.multiple_of(h * HEAD_DIM, HEAD_DIM), HEAD_DIM)


def each_head(q_ref, body):
    def one(h, unused):
        body(h, head_cols(h))
        return unused

    lax.fori_loop(0, q_ref.shape[1] // HEAD_DIM, one, 0)


def chunk_part(off_ref, q_ref, k_ref, v_ref, h, carry, masked):
    rows, span = q_ref.shape[0], 256
    cols = head_cols(h)
    from_s = lax.broadcasted_iota(jnp.int32, (span, span), 0)
    to_s = lax.broadcasted_iota(jnp.int32, (span, span), 1)
    later = (from_s >= to_s).astype(jnp.float32).astype(jnp.bfloat16)
    q = q_ref[:, cols]
    total = None
    for start in reversed(range(0, k_ref.shape[0], span)):
        strict = None
        if masked:
            at_q = lax.broadcasted_iota(jnp.int32, (rows, span), 0)
            at_k = lax.broadcasted_iota(jnp.int32, (rows, span), 1) + start
            strict = at_k < at_q
        part, carry = key_tile(
            q, k_ref[start:start + span, cols], v_ref[start:start + span, cols],
            off_ref[h], later, carry, strict,
        )
        total = part if total is None else total + part
    return total, carry


def wide(column):
    return jnp.broadcast_to(column, (column.shape[0], HEAD_DIM))


def own_chunk_body(off_ref, q_ref, k_ref, v_ref, near_ref, carry_ref):
    def one(h, cols):
        zero = jnp.zeros((q_ref.shape[0], 1), jnp.float32)
        part, carry = chunk_part(off_ref, q_ref, k_ref, v_ref, h, zero, True)
        near_ref[:, cols] = part
        carry_ref[:, cols] = wide(carry)

    each_head(q_ref, one)


def near_update(off_ref, q_ref, k_ref, v_ref, near_in, carry_in, near_ref, carry_ref):
    def one(h, cols):
        part, carry = chunk_part(off_ref, q_ref, k_ref, v_ref, h, carry_in[:, cols][:, :1], False)
        near_ref[:, cols] = near_in[:, cols] + part
        carry_ref[:, cols] = wide(carry)

    each_head(q_ref, one)


def far_update(off_ref, q_ref, k_ref, v_ref, far_in, far_ref):
    def one(h, cols):
        zero = jnp.zeros((q_ref.shape[0], 1), jnp.float32)
        part, carry = chunk_part(off_ref, q_ref, k_ref, v_ref, h, zero, False)
        far_ref[:, cols] = part + far_in[:, cols] * jnp.exp2(-carry)

    each_head(q_ref, one)


def hop_body(hop, places, first, place_ref, off_ref, q_ref, kn, vn, kf, vf, near_in, carry_in, *rest):
    if first:
        near_ref, carry_ref, far_ref = rest
    else:
        far_in, near_ref, carry_ref, far_ref = rest

    @pl.when(place_ref[0] >= hop)
    def _():
        near_update(off_ref, q_ref, kn, vn, near_in, carry_in, near_ref, carry_ref)

    @pl.when(place_ref[0] < hop)
    def _():
        near_ref[...] = near_in[...]
        carry_ref[...] = carry_in[...]

    if first:
        far_ref[...] = jnp.zeros_like(far_ref)
        far_in = far_ref

    @pl.when(place_ref[0] + hop >= places)
    def _():
        far_update(off_ref, q_ref, kf, vf, far_in, far_ref)

    if not first:
        @pl.when(place_ref[0] + hop < places)
        def _():
            far_ref[...] = far_in[...]


def last_body(hop, place_ref, off_ref, q_ref, kn, vn, near_in, carry_in, far_in, out_ref, near_ref, carry_ref):
    near_ref[...] = near_in[...]
    carry_ref[...] = carry_in[...]

    @pl.when(place_ref[0] >= hop)
    def _():
        near_update(off_ref, q_ref, kn, vn, near_in, carry_in, near_ref, carry_ref)

    out_ref[...] = (near_ref[...] + jnp.exp2(-carry_ref[...]) * far_in[...]).astype(jnp.bfloat16)


def run_local(body, name, scalars, arrays, outs, scratch=(), chunks=1):
    smem = pl.BlockSpec(memory_space=pltpu.SMEM)
    vmem = pl.BlockSpec(memory_space=pltpu.VMEM)
    rows, width = arrays[0].shape
    tiles = chunks * rows * arrays[1].shape[0] * (width // HEAD_DIM)
    return pl.pallas_call(
        body,
        in_specs=[smem] * len(scalars) + [vmem] * len(arrays),
        out_specs=jax.tree.map(lambda _: vmem, outs),
        out_shape=outs,
        scratch_shapes=list(scratch),
        cost_estimate=pl.CostEstimate(flops=tiles * 2 * 2 * (HEAD_DIM + HEAD_DIM), transcendentals=3 * tiles, bytes_accessed=4 * rows * width),
        name=name,
    )(*scalars, *arrays)


def ring_attend(queries, keys, values, offsets):
    devices = lax.axis_size("sp")
    places = devices // 2
    me = lax.axis_index("sp").astype(jnp.int32)
    core, place = me % 2, me // 2
    heads = offsets.shape[0] // 2
    half = heads * HEAD_DIM
    mate = [(i, i ^ 1) for i in range(devices)]

    def split(a):
        low, high = a[:, :half], a[:, half:]
        return jnp.where(core == 0, low, high), jnp.where(core == 0, high, low)

    def traded(a):
        kept, given = split(a)
        got = lax.ppermute(given, "sp", mate)
        return jnp.concatenate([jnp.where(core == 0, kept, got), jnp.where(core == 0, got, kept)], axis=0)

    k, v, q = traded(keys), traded(values), traded(queries)
    off = jnp.where(core == 0, offsets[:heads], offsets[heads:])
    state = jax.ShapeDtypeStruct((q.shape[0], half), jnp.float32)
    up = [(i, (i + 2) % devices) for i in range(devices)]
    down = [(i, (i - 2) % devices) for i in range(devices)]
    near, carry = run_local(own_chunk_body, "own_chunk", (off,), (q, k, v), (state, state))
    near_hops = places // 2
    far_hops = places - 1 - near_hops
    place = place.reshape(1)
    near_now = tuple(lax.ppermute(a, "sp", up) for a in (k, v))
    far_now = tuple(lax.ppermute(a, "sp", down) for a in (k, v))
    far = None
    for hop in range(1, near_hops + 1):
        near_next, far_next = [], []
        for i in range(2):
            if hop < far_hops or (hop < near_hops and i == 0):
                tied, near = lax.optimization_barrier((near_now[i], near))
                near_next.append(lax.ppermute(tied, "sp", up))
            if hop < far_hops or (hop < near_hops and i == 1):
                tied, near = lax.optimization_barrier((far_now[i], near))
                far_next.append(lax.ppermute(tied, "sp", down))
        if hop <= far_hops:
            first = far is None
            near, carry, far = run_local(
                functools.partial(hop_body, hop, places, first), "hop",
                (place, off), (q, *near_now, *far_now, near, carry) + (() if first else (far,)),
                (state, state, state), chunks=2,
            )
        else:
            out = jax.ShapeDtypeStruct(q.shape, jnp.bfloat16)
            attended = run_local(
                functools.partial(last_body, hop), "last_hop",
                (place, off), (q, *near_now, *far_now, near, carry, far), out,
                scratch=(pltpu.VMEM(state.shape, jnp.float32), pltpu.VMEM(state.shape, jnp.float32)),
            )
        near_now, far_now = near_next, far_next
    rows = queries.shape[0]
    first_rows, second_rows = attended[:rows], attended[rows:]
    kept = jnp.where(core == 0, first_rows, second_rows)
    got = lax.ppermute(jnp.where(core == 0, second_rows, first_rows), "sp", mate)
    return jnp.where(core == 0, jnp.concatenate([kept, got], axis=1), jnp.concatenate([got, kept], axis=1))


def projected_and_sent(rows, weight, axis):
    peers = lax.axis_size(axis)
    me = lax.axis_index(axis)
    count = rows.shape[0] // peers
    away = sorted(range(peers), key=lambda d: -min(d, peers - d))
    arrived = []
    for d in away:
        mine = lax.dynamic_slice_in_dim(rows, lax.rem(me + d, peers) * count, count, 0)
        part = jnp.dot(mine, weight, preferred_element_type=jnp.float32).astype(jnp.bfloat16)
        if d:
            part = lax.ppermute(part, axis, [(i, (i + d) % peers) for i in range(peers)])
        arrived.append(part)
    return arrived


def normalised(rows, gain, shift):
    mean = jnp.mean(rows, axis=-1, keepdims=True)
    centred = rows - mean
    variance = jnp.mean(centred * centred, axis=-1, keepdims=True)
    return centred * lax.rsqrt(variance + norm_eps) * gain + shift


def send_body(target_ref, residual_ref, gain_ref, shift_ref, *rest):
    *tile_refs, normed_ref, buffer_ref = rest
    mixed = tile_refs[0][...].astype(jnp.float32)
    for tile_ref in tile_refs[1:]:
        mixed = mixed + tile_ref[...].astype(jnp.float32)
    rows = residual_scale * residual_ref[...].astype(jnp.float32) + mixed
    normed = normalised(rows, gain_ref[...], shift_ref[...]).astype(jnp.bfloat16)
    normed_ref[...] = normed
    width = buffer_ref.shape[1]
    pieces = jnp.concatenate(
        [normed[:, start:start + width] for start in range(0, normed.shape[1], width)], axis=0
    )
    first, second = target_ref[0:1, :], target_ref[1:2, :]
    block = 256

    def fill(n, unused):
        start = pl.multiple_of(n * block, block)
        at = lax.broadcasted_iota(jnp.int32, (block, pieces.shape[0]), 0) + start
        chosen = ((at == first) | (at == second)).astype(jnp.float32).astype(jnp.bfloat16)
        buffer_ref[pl.ds(start, block), :] = jnp.dot(
            chosen, pieces, preferred_element_type=jnp.float32
        ).astype(jnp.bfloat16)
        return unused

    lax.fori_loop(0, buffer_ref.shape[0] // block, fill, 0)


def receive_body(meta_ref, returned_ref, normed_ref, gain_ref, shift_ref, out_ref, one_ref, two_ref):
    count, width = meta_ref.shape[0], returned_ref.shape[1]
    first = meta_ref[:, 0:1].astype(jnp.int32)
    second = meta_ref[:, 1:2].astype(jnp.int32)
    block = 256
    one_ref[...] = jnp.zeros_like(one_ref)
    two_ref[...] = jnp.zeros_like(two_ref)

    def pick(n, unused):
        start = pl.multiple_of(n * block, block)
        at = lax.broadcasted_iota(jnp.int32, (count, block), 1) + start
        rows = returned_ref[pl.ds(start, block), :]
        for target, total_ref in ((first, one_ref), (second, two_ref)):
            chosen = (at == target).astype(jnp.float32).astype(jnp.bfloat16)
            total_ref[...] += jnp.dot(chosen, rows, preferred_element_type=jnp.float32)
        return unused

    lax.fori_loop(0, returned_ref.shape[0] // block, pick, 0)
    moe = meta_ref[:, 2:3] * one_ref[...] + meta_ref[:, 3:4] * two_ref[...]
    tokens = normed_ref.shape[0]
    moe = jnp.concatenate([moe[start:start + tokens] for start in range(0, count, tokens)], axis=1)
    rows = residual_scale * normed_ref[...].astype(jnp.float32) + moe
    out_ref[...] = normalised(rows, gain_ref[...], shift_ref[...]).astype(jnp.bfloat16)


def whole(body, name, arrays, outs, scratch=()):
    vmem = pl.BlockSpec(memory_space=pltpu.VMEM)
    return pl.pallas_call(
        body,
        in_specs=[vmem] * len(arrays),
        out_specs=jax.tree.map(lambda _: vmem, outs),
        out_shape=outs,
        scratch_shapes=list(scratch),
        name=name,
    )(*arrays)


def slot_index(routes, expert_count, capacity):
    flat = routes.reshape(-1)
    onehot = (flat[:, None] == jnp.arange(expert_count, dtype=jnp.int32)[None, :]).astype(jnp.int32)
    earlier = jnp.cumsum(onehot, axis=0) - onehot
    rank = jnp.sum(earlier * onehot, axis=1)
    return flat * capacity + rank


def expert_body(arrived_ref, gate_ref, up_ref, down_ref, out_ref, spread_ref):
    count, piece = arrived_ref.shape
    cuts = down_ref.shape[1] // piece
    rows = count // cuts
    lanes = piece // spread_ref.shape[0]

    def each(work):
        def one(n, unused):
            at = pl.ds(pl.multiple_of(n * rows, rows), rows)
            for c in range(spread_ref.shape[0]):
                work(at, c, slice(c * lanes, (c + 1) * lanes))
            return unused

        lax.fori_loop(0, cuts, one, 0)

    def widen(at, c, cols):
        spread_ref[c, at, :] = arrived_ref[at, cols].astype(jnp.float32)

    def narrow(at, c, cols):
        out_ref[at, cols] = spread_ref[c, at, :].astype(jnp.bfloat16)

    each(widen)
    gate, upper = None, None
    for k in range(cuts):
        x = jnp.concatenate(
            [spread_ref[c, pl.ds(k, rows, stride=cuts), :] for c in range(spread_ref.shape[0])], axis=1
        ).astype(jnp.bfloat16)
        part = slice(k * piece, (k + 1) * piece)
        more = jnp.dot(x, gate_ref[part, :], preferred_element_type=jnp.float32)
        gate = more if gate is None else gate + more
        more = jnp.dot(x, up_ref[part, :], preferred_element_type=jnp.float32)
        upper = more if upper is None else upper + more
    hidden = (gate / (1.0 + jnp.exp(-gate)) * upper).astype(jnp.bfloat16)
    for k in range(cuts):
        made = jnp.dot(hidden, down_ref[:, k * piece:(k + 1) * piece], preferred_element_type=jnp.float32)
        for c in range(spread_ref.shape[0]):
            spread_ref[c, pl.ds(k, rows, stride=cuts), :] = made[:, c * lanes:(c + 1) * lanes]
    each(narrow)


def per_device(
    queries,
    keys,
    values,
    offsets,
    residual,
    out_weight,
    gain_one,
    shift_one,
    gain_two,
    shift_two,
    group_prob,
    pair_logits,
    routes,
    w_gate,
    w_up,
    w_down,
):
    attended_rows = ring_attend(queries, keys, values, offsets)
    local_rows = residual.shape[0]
    width = residual.shape[1]
    expert_count = lax.axis_size("sp") * lax.axis_size("tp")
    capacity = local_rows // (expert_count // GROUPS)
    slot_count = expert_count * capacity
    cuts = 16 // capacity
    piece = width // cuts
    slots = slot_index(routes, expert_count, capacity).reshape(local_rows, TOPK)
    cut = jnp.arange(cuts, dtype=jnp.int32)[None, :, None]
    targets = (slots.T[:, None, :] * cuts + cut).reshape(TOPK, cuts * local_rows)
    difference = pair_logits[:, 0] - pair_logits[:, 1]
    pair_weight = jnp.stack([jax.nn.sigmoid(difference), jax.nn.sigmoid(-difference)], axis=0)
    route_weight = jnp.tile(group_prob[None, :] * pair_weight, (1, cuts))
    meta = jnp.concatenate([targets.astype(jnp.float32), route_weight], axis=0).T
    tiles = projected_and_sent(attended_rows, out_weight, "tp")
    buffer_shape = jax.ShapeDtypeStruct((slot_count * cuts, piece), jnp.bfloat16)
    rows_shape = jax.ShapeDtypeStruct((local_rows, width), jnp.bfloat16)
    normed, buffer = whole(
        send_body, "norm_and_place",
        (targets, residual, gain_one[None, :], shift_one[None, :], *tiles), (rows_shape, buffer_shape),
    )
    arrived = lax.all_to_all(buffer, ("sp", "tp"), split_axis=0, concat_axis=0, tiled=True)
    result = whole(
        expert_body, "expert", (arrived, w_gate[0], w_up[0], w_down[0]), buffer_shape,
        (pltpu.VMEM((piece // HEAD_DIM, slot_count * cuts, HEAD_DIM), jnp.float32),),
    )
    returned = lax.all_to_all(result, ("sp", "tp"), split_axis=0, concat_axis=0, tiled=True)
    picked = pltpu.VMEM((cuts * local_rows, piece), jnp.float32)
    return whole(
        receive_body, "pick_and_norm",
        (meta, returned, normed, gain_two[None, :], shift_two[None, :]), rows_shape, (picked, picked),
    )


def solution(mesh):
    return jax.shard_map(
        per_device,
        mesh=mesh,
        in_specs=(
            P(("grp", "sp"), "tp"),
            P(("grp", "sp"), "tp"),
            P(("grp", "sp"), "tp"),
            P("tp"),
            P(("grp", "sp", "tp"), None),
            P("tp", None),
            P(),
            P(),
            P(),
            P(),
            P(("grp", "sp", "tp")),
            P(("grp", "sp", "tp"), None),
            P(("grp", "sp", "tp"), None),
            P(("sp", "tp"), None, None),
            P(("sp", "tp"), None, None),
            P(("sp", "tp"), None, None),
        ),
        out_specs=P(("grp", "sp", "tp"), None),
        check_vma=False,
    )
```

```python
import functools
import jax
import jax.numpy as jnp
from jax import lax
from jax.experimental import pallas as pl
from jax.experimental.pallas import tpu as pltpu
from jax.sharding import PartitionSpec as P

HEAD_DIM = 128
GROUPS = 4
TOPK = 2


residual_scale = 8.0**0.25
norm_eps = 1e-05


LOG2E = 1.4426950408889634
EXP_CAP = 126.0


def key_tile(q, k, v, offset, later, carry, strict):
    score = lax.dot_general(q, k, (((1,), (1,)), ((), ())), preferred_element_type=jnp.float32)
    y = score * (HEAD_DIM ** (-0.5) * LOG2E) - offset * LOG2E
    soft = jnp.maximum(y, jnp.log(1.0 + jnp.exp2(jnp.minimum(y, EXP_CAP))) * LOG2E)
    if strict is not None:
        soft = jnp.where(strict, soft, 0.0)
    sums = jnp.dot(soft.astype(jnp.bfloat16), later, preferred_element_type=jnp.float32)
    weight = jnp.exp2(y - carry - sums)
    if strict is not None:
        weight = jnp.where(strict, weight, 0.0)
    part = jnp.dot(weight.astype(jnp.bfloat16), v, preferred_element_type=jnp.float32)
    return part, carry + sums[:, :1]


def head_cols(h):
    return pl.ds(pl.multiple_of(h * HEAD_DIM, HEAD_DIM), HEAD_DIM)


def each_head(q_ref, body):
    def one(h, unused):
        body(h, head_cols(h))
        return unused

    lax.fori_loop(0, q_ref.shape[1] // HEAD_DIM, one, 0)


def chunk_part(place_ref, off_ref, q_ref, k_ref, v_ref, h, carry, masked):
    rows, span = q_ref.shape[0], 256
    cols = head_cols(h)
    from_s = lax.broadcasted_iota(jnp.int32, (span, span), 0)
    to_s = lax.broadcasted_iota(jnp.int32, (span, span), 1)
    later = (from_s >= to_s).astype(jnp.float32).astype(jnp.bfloat16)
    q = q_ref[:, cols]
    total = None
    for start in reversed(range(0, k_ref.shape[0], span)):
        strict = None
        if masked:
            at_q = lax.broadcasted_iota(jnp.int32, (rows, span), 0)
            at_k = lax.broadcasted_iota(jnp.int32, (rows, span), 1) + start
            strict = at_k < at_q
        part, carry = key_tile(
            q, k_ref[start:start + span, cols], v_ref[start:start + span, cols],
            off_ref[place_ref[1] * (q_ref.shape[1] // HEAD_DIM) + h], later, carry, strict,
        )
        total = part if total is None else total + part
    return total, carry


def wide(column):
    return jnp.broadcast_to(column, (column.shape[0], HEAD_DIM))


def own_chunk_body(place_ref, off_ref, q_ref, k_ref, v_ref, near_ref, carry_ref):
    def one(h, cols):
        zero = jnp.zeros((q_ref.shape[0], 1), jnp.float32)
        part, carry = chunk_part(place_ref, off_ref, q_ref, k_ref, v_ref, h, zero, True)
        near_ref[:, cols] = part
        carry_ref[:, cols] = wide(carry)

    each_head(q_ref, one)


def near_update(place_ref, off_ref, q_ref, k_ref, v_ref, near_in, carry_in, near_ref, carry_ref):
    def one(h, cols):
        part, carry = chunk_part(place_ref, off_ref, q_ref, k_ref, v_ref, h, carry_in[:, cols][:, :1], False)
        near_ref[:, cols] = near_in[:, cols] + part
        carry_ref[:, cols] = wide(carry)

    each_head(q_ref, one)


def far_update(place_ref, off_ref, q_ref, k_ref, v_ref, far_in, far_ref):
    def one(h, cols):
        zero = jnp.zeros((q_ref.shape[0], 1), jnp.float32)
        part, carry = chunk_part(place_ref, off_ref, q_ref, k_ref, v_ref, h, zero, False)
        far_ref[:, cols] = part + far_in[:, cols] * jnp.exp2(-carry)

    each_head(q_ref, one)


def hop_body(hop, places, first, place_ref, off_ref, q_ref, kn, vn, kf, vf, near_in, carry_in, *rest):
    if first:
        near_ref, carry_ref, far_ref = rest
    else:
        far_in, near_ref, carry_ref, far_ref = rest

    @pl.when(place_ref[0] >= hop)
    def _():
        near_update(place_ref, off_ref, q_ref, kn, vn, near_in, carry_in, near_ref, carry_ref)

    @pl.when(place_ref[0] < hop)
    def _():
        near_ref[...] = near_in[...]
        carry_ref[...] = carry_in[...]

    if first:
        far_ref[...] = jnp.zeros_like(far_ref)
        far_in = far_ref

    @pl.when(place_ref[0] + hop >= places)
    def _():
        far_update(place_ref, off_ref, q_ref, kf, vf, far_in, far_ref)

    if not first:
        @pl.when(place_ref[0] + hop < places)
        def _():
            far_ref[...] = far_in[...]


def last_body(hop, place_ref, off_ref, q_ref, kn, vn, near_in, carry_in, far_in, kept_ref, given_ref, near_ref, carry_ref):
    near_ref[...] = near_in[...]
    carry_ref[...] = carry_in[...]

    @pl.when(place_ref[0] >= hop)
    def _():
        near_update(place_ref, off_ref, q_ref, kn, vn, near_in, carry_in, near_ref, carry_ref)

    rows = kept_ref.shape[0]
    for target_ref, half in ((kept_ref, place_ref[1]), (given_ref, 1 - place_ref[1])):
        at = pl.ds(pl.multiple_of(half * rows, rows), rows)
        target_ref[...] = (near_ref[at, :] + jnp.exp2(-carry_ref[at, :]) * far_in[at, :]).astype(jnp.bfloat16)


def run_local(body, name, scalars, arrays, outs, scratch=(), chunks=1):
    smem = pl.BlockSpec(memory_space=pltpu.SMEM)
    vmem = pl.BlockSpec(memory_space=pltpu.VMEM)
    rows, width = arrays[0].shape
    tiles = chunks * rows * arrays[1].shape[0] * (width // HEAD_DIM)
    return pl.pallas_call(
        body,
        in_specs=[smem] * len(scalars) + [vmem] * len(arrays),
        out_specs=jax.tree.map(lambda _: vmem, outs),
        out_shape=outs,
        scratch_shapes=list(scratch),
        cost_estimate=pl.CostEstimate(flops=tiles * 2 * 2 * (HEAD_DIM + HEAD_DIM), transcendentals=3 * tiles, bytes_accessed=4 * rows * width),
        name=name,
    )(*scalars, *arrays)


def ring_attend(queries, keys, values, offsets):
    devices = lax.axis_size("sp")
    places = devices // 2
    me = lax.axis_index("sp").astype(jnp.int32)
    core, place = me % 2, me // 2
    heads = offsets.shape[0] // 2
    half = heads * HEAD_DIM
    mate = [(i, i ^ 1) for i in range(devices)]

    def split(a):
        low, high = a[:, :half], a[:, half:]
        return jnp.where(core == 0, low, high), jnp.where(core == 0, high, low)

    def traded(a):
        kept, given = split(a)
        got = lax.ppermute(given, "sp", mate)
        return jnp.concatenate([jnp.where(core == 0, kept, got), jnp.where(core == 0, got, kept)], axis=0)

    k, v, q = traded(keys), traded(values), traded(queries)
    state = jax.ShapeDtypeStruct((q.shape[0], half), jnp.float32)
    up = [(i, (i + 2) % devices) for i in range(devices)]
    down = [(i, (i - 2) % devices) for i in range(devices)]
    spot = jnp.stack([place, core])
    near, carry = run_local(own_chunk_body, "own_chunk", (spot, offsets), (q, k, v), (state, state))
    near_hops = places // 2
    far_hops = places - 1 - near_hops
    near_now = tuple(lax.ppermute(a, "sp", up) for a in (k, v))
    far_now = tuple(lax.ppermute(a, "sp", down) for a in (k, v))
    far = None
    for hop in range(1, near_hops + 1):
        near_next, far_next = [], []
        for i in range(2):
            if hop < far_hops or (hop < near_hops and i == 0):
                tied, near = lax.optimization_barrier((near_now[i], near))
                near_next.append(lax.ppermute(tied, "sp", up))
            if hop < far_hops or (hop < near_hops and i == 1):
                tied, near = lax.optimization_barrier((far_now[i], near))
                far_next.append(lax.ppermute(tied, "sp", down))
        if hop <= far_hops:
            first = far is None
            near, carry, far = run_local(
                functools.partial(hop_body, hop, places, first), "hop",
                (spot, offsets), (q, *near_now, *far_now, near, carry) + (() if first else (far,)),
                (state, state, state), chunks=2,
            )
        else:
            out = jax.ShapeDtypeStruct((queries.shape[0], half), jnp.bfloat16)
            kept, given = run_local(
                functools.partial(last_body, hop), "last_hop",
                (spot, offsets), (q, *near_now, *far_now, near, carry, far), (out, out),
                scratch=(pltpu.VMEM(state.shape, jnp.float32), pltpu.VMEM(state.shape, jnp.float32)),
            )
        near_now, far_now = near_next, far_next
    got = lax.ppermute(given, "sp", mate)
    return jnp.where(core == 0, jnp.concatenate([kept, got], axis=1), jnp.concatenate([got, kept], axis=1))


def projected_and_sent(rows, weight, axis):
    peers = lax.axis_size(axis)
    me = lax.axis_index(axis)
    count = rows.shape[0] // peers
    away = sorted(range(peers), key=lambda d: -min(d, peers - d))
    arrived = []
    for d in away:
        mine = lax.dynamic_slice_in_dim(rows, lax.rem(me + d, peers) * count, count, 0)
        part = jnp.dot(mine, weight, preferred_element_type=jnp.float32).astype(jnp.bfloat16)
        if d:
            part = lax.ppermute(part, axis, [(i, (i + d) % peers) for i in range(peers)])
        arrived.append(part)
    return arrived


def normalised(rows, gain, shift):
    mean = jnp.mean(rows, axis=-1, keepdims=True)
    centred = rows - mean
    variance = jnp.mean(centred * centred, axis=-1, keepdims=True)
    return centred * lax.rsqrt(variance + norm_eps) * gain + shift


def each_block(spread_ref, block, work):
    chunks, rows, lanes = spread_ref.shape

    def one(n, unused):
        at = pl.ds(pl.multiple_of(n * block, block), block)
        for c in range(chunks):
            work(at, c, slice(c * lanes, (c + 1) * lanes))
        return unused

    lax.fori_loop(0, rows // block, one, 0)


def widen_into(spread_ref, source_ref, block):
    def work(at, c, cols):
        spread_ref[c, at, :] = source_ref[at, cols].astype(jnp.float32)

    each_block(spread_ref, block, work)


def narrow_from(spread_ref, target_ref, block):
    def work(at, c, cols):
        target_ref[at, cols] = spread_ref[c, at, :].astype(jnp.bfloat16)

    each_block(spread_ref, block, work)


def piece_rows(spread_ref, k, rows, cuts):
    parts = [spread_ref[c, pl.ds(k, rows, stride=cuts), :] for c in range(spread_ref.shape[0])]
    return jnp.concatenate(parts, axis=1).astype(jnp.bfloat16)


def put_piece_rows(spread_ref, k, value, cuts):
    lanes = spread_ref.shape[2]
    for c in range(spread_ref.shape[0]):
        spread_ref[c, pl.ds(k, value.shape[0], stride=cuts), :] = value[:, c * lanes:(c + 1) * lanes]


def send_body(target_ref, residual_ref, gain_ref, shift_ref, *rest):
    *tile_refs, normed_ref, buffer_ref, spread_ref = rest
    mixed = tile_refs[0][...].astype(jnp.float32)
    for tile_ref in tile_refs[1:]:
        mixed = mixed + tile_ref[...].astype(jnp.float32)
    rows = residual_scale * residual_ref[...].astype(jnp.float32) + mixed
    normed_ref[...] = normalised(rows, gain_ref[...], shift_ref[...]).astype(jnp.bfloat16)
    piece = buffer_ref.shape[1]
    cuts = normed_ref.shape[1] // piece
    slot_count = buffer_ref.shape[0] // cuts
    at = lax.broadcasted_iota(jnp.int32, (slot_count, normed_ref.shape[0]), 0)
    chosen = (at == target_ref[0:1, :]) | (at == target_ref[1:2, :])
    chosen = chosen.astype(jnp.float32).astype(jnp.bfloat16)
    for k in range(cuts):
        part = normed_ref[:, k * piece:(k + 1) * piece]
        put_piece_rows(spread_ref, k, jnp.dot(chosen, part, preferred_element_type=jnp.float32), cuts)
    narrow_from(spread_ref, buffer_ref, slot_count)


def receive_body(meta_ref, returned_ref, normed_ref, gain_ref, shift_ref, out_ref, spread_ref):
    tokens, width = normed_ref.shape
    cuts = width // returned_ref.shape[1]
    slot_count = returned_ref.shape[0] // cuts
    widen_into(spread_ref, returned_ref, slot_count)
    at = lax.broadcasted_iota(jnp.int32, (tokens, slot_count), 1)
    chosen = jnp.concatenate(
        [(at == meta_ref[:, i:i + 1].astype(jnp.int32)).astype(jnp.float32) for i in range(2)], axis=0
    ).astype(jnp.bfloat16)
    moe = []
    for k in range(cuts):
        both = jnp.dot(
            chosen, piece_rows(spread_ref, k, slot_count, cuts), preferred_element_type=jnp.float32
        )
        moe.append(meta_ref[:, 2:3] * both[:tokens] + meta_ref[:, 3:4] * both[tokens:])
    rows = residual_scale * normed_ref[...].astype(jnp.float32) + jnp.concatenate(moe, axis=1)
    out_ref[...] = normalised(rows, gain_ref[...], shift_ref[...]).astype(jnp.bfloat16)


def whole(body, name, arrays, outs, scratch=()):
    vmem = pl.BlockSpec(memory_space=pltpu.VMEM)
    return pl.pallas_call(
        body,
        in_specs=[vmem] * len(arrays),
        out_specs=jax.tree.map(lambda _: vmem, outs),
        out_shape=outs,
        scratch_shapes=list(scratch),
        name=name,
    )(*arrays)


def slot_index(routes, expert_count, capacity):
    flat = routes.reshape(-1)
    onehot = (flat[:, None] == jnp.arange(expert_count, dtype=jnp.int32)[None, :]).astype(jnp.int32)
    earlier = jnp.cumsum(onehot, axis=0) - onehot
    rank = jnp.sum(earlier * onehot, axis=1)
    return flat * capacity + rank


def expert_body(arrived_ref, gate_ref, up_ref, down_ref, out_ref, spread_ref):
    count, piece = arrived_ref.shape
    cuts = down_ref.shape[1] // piece
    rows = count // cuts
    widen_into(spread_ref, arrived_ref, rows)
    gate, upper = None, None
    for k in range(cuts):
        x = piece_rows(spread_ref, k, rows, cuts)
        part = slice(k * piece, (k + 1) * piece)
        more = jnp.dot(x, gate_ref[part, :], preferred_element_type=jnp.float32)
        gate = more if gate is None else gate + more
        more = jnp.dot(x, up_ref[part, :], preferred_element_type=jnp.float32)
        upper = more if upper is None else upper + more
    hidden = (gate / (1.0 + jnp.exp(-gate)) * upper).astype(jnp.bfloat16)
    for k in range(cuts):
        made = jnp.dot(hidden, down_ref[:, k * piece:(k + 1) * piece], preferred_element_type=jnp.float32)
        put_piece_rows(spread_ref, k, made, cuts)
    narrow_from(spread_ref, out_ref, rows)


def per_device(
    queries,
    keys,
    values,
    offsets,
    residual,
    out_weight,
    gain_one,
    shift_one,
    gain_two,
    shift_two,
    group_prob,
    pair_logits,
    routes,
    w_gate,
    w_up,
    w_down,
):
    attended_rows = ring_attend(queries, keys, values, offsets)
    local_rows = residual.shape[0]
    width = residual.shape[1]
    expert_count = lax.axis_size("sp") * lax.axis_size("tp")
    capacity = local_rows // (expert_count // GROUPS)
    slot_count = expert_count * capacity
    cuts = 16 // capacity
    piece = width // cuts
    slots = slot_index(routes, expert_count, capacity).reshape(local_rows, TOPK)
    targets = slots.T
    difference = pair_logits[:, 0] - pair_logits[:, 1]
    pair_weight = jnp.stack([jax.nn.sigmoid(difference), jax.nn.sigmoid(-difference)], axis=1)
    route_weight = group_prob[:, None] * pair_weight
    meta = jnp.concatenate([slots.astype(jnp.float32), route_weight], axis=1)
    spread = pltpu.VMEM((piece // HEAD_DIM, slot_count * cuts, HEAD_DIM), jnp.float32)
    tiles = projected_and_sent(attended_rows, out_weight, "tp")
    buffer_shape = jax.ShapeDtypeStruct((slot_count * cuts, piece), jnp.bfloat16)
    rows_shape = jax.ShapeDtypeStruct((local_rows, width), jnp.bfloat16)
    normed, buffer = whole(
        send_body, "norm_and_place",
        (targets, residual, gain_one[None, :], shift_one[None, :], *tiles), (rows_shape, buffer_shape), (spread,),
    )
    arrived = lax.all_to_all(buffer, ("sp", "tp"), split_axis=0, concat_axis=0, tiled=True)
    result = whole(
        expert_body, "expert", (arrived, w_gate[0], w_up[0], w_down[0]), buffer_shape,
        (spread,),
    )
    returned = lax.all_to_all(result, ("sp", "tp"), split_axis=0, concat_axis=0, tiled=True)
    return whole(
        receive_body, "pick_and_norm",
        (meta, returned, normed, gain_two[None, :], shift_two[None, :]), rows_shape, (spread,),
    )


def solution(mesh):
    return jax.shard_map(
        per_device,
        mesh=mesh,
        in_specs=(
            P(("grp", "sp"), "tp"),
            P(("grp", "sp"), "tp"),
            P(("grp", "sp"), "tp"),
            P("tp"),
            P(("grp", "sp", "tp"), None),
            P("tp", None),
            P(),
            P(),
            P(),
            P(),
            P(("grp", "sp", "tp")),
            P(("grp", "sp", "tp"), None),
            P(("grp", "sp", "tp"), None),
            P(("sp", "tp"), None, None),
            P(("sp", "tp"), None, None),
            P(("sp", "tp"), None, None),
        ),
        out_specs=P(("grp", "sp", "tp"), None),
        check_vma=False,
    )
```
